256 devices in a mesh: sp: 32 (over z, x), tp: 8 (over y, core).
Axes of the slice: x: 4, y: 4, z: 8, core: 2. Of those that a mesh axis runs over, the one named last changes fastest.
Arguments:
- layer_input: bfloat16 [16, 16384, 2048], P(None, ('sp', 'tp')), as said below
- key_weight: bfloat16 [2048, 384], replicated, may hold values from -0.125 to 0.125
- value_weight: bfloat16 [2048, 384], replicated, may hold values from -0.125 to 0.125
- queries: bfloat16 [96, 5, 64], P('sp'), may hold values from -6 to 6
- head_bias: float32 [6, 5], replicated, as said below
Outputs:
- stored: bfloat16 [96, 32, 512, 128], P('sp', None, 'tp')
- first_read: bfloat16 [96, 320], P('sp')
The draws below stay inside these ranges and needn't reach their ends.
Inputs may be any that keep to these rules, and one draw needn't show every extreme that they name: `layer_input`: entries lie between -12.5 and 12.5. `head_bias`: entries lie between -1 minus the natural logarithm of 16384 and -3.
All inputs are finite; a program needn't handle non-finite values.
Results may differ from the reference program's by a relative error of at most 0.01.
Values may be sent and summed in bfloat16 or wider, within the bound.
No kernel may reach another device: no remote copies, remote signals or barrier semaphores. Data moves between devices by JAX's collectives and lax.ppermute only.
A program may use at most 64 MiB of HBM per device.

```python
import math
import jax
import jax.numpy as jnp
from jax import lax

D = 2048
HD = 64
KVH = 6
GROUP = 5
SUB = 64
SEQS = 16
PAIRS = 96
LEN = 16384
BLOCKS = 32
SPAN = 512


def draw_layer_input(key, part):
    base_key, scale_key = jax.random.split(key)
    blocks = LEN // SUB
    log_scale = jax.random.uniform(scale_key, (SEQS, blocks, 1, 1), jnp.float32, -0.7, 0.7)
    base = jnp.clip(jax.random.normal(base_key, (SEQS, blocks, SUB, D), jnp.float32), -6.0, 6.0)
    return (base * jnp.exp(log_scale)).reshape(SEQS, LEN, D).astype(jnp.bfloat16)


def draw_head_bias(key, part):
    kind_key, fast_key, slow_key = jax.random.split(key, 3)
    quick = jax.random.randint(kind_key, (KVH, GROUP), 0, 2) == 1
    fast = -math.log(40.0) + jax.random.uniform(fast_key, (KVH, GROUP), jnp.float32, -0.5, 0.5)
    slow = -math.log(LEN) - 0.5 + jax.random.uniform(slow_key, (KVH, GROUP), jnp.float32, -0.5, 0.5)
    return jnp.where(quick, fast, slow).astype(jnp.float32)


def shard_levels(rng, dims, cuts, least, top_value):
    def one(axis_at, parts):
        steps = jax.random.uniform(jax.random.fold_in(jax.random.fold_in(rng, 6), axis_at), (parts,), jnp.float32, least / len(cuts), top_value / len(cuts))
        return jnp.repeat(jnp.exp(steps), dims[axis_at] // parts).reshape((-1,) + (1,) * (len(dims) - axis_at - 1))

    level = one(*cuts[0])
    for cut in cuts[1:]:
        level = level * one(*cut)
    return level


def noise(own_key, dims, scale, most, cuts=(), held_as=jnp.bfloat16):
    factor_of = shard_levels(own_key, dims, cuts, -0.22, 0.18) if cuts else 1.0
    array = jax.random.normal(own_key, dims, jnp.float32) * scale * factor_of
    return jnp.minimum(jnp.maximum(array, -most), most).astype(held_as)


def setup_inputs(seed: int = 0) -> dict:
    streams_of = jax.random.split(jax.random.key(seed), 6)
    return {
        "layer_input": draw_layer_input(jax.random.fold_in(streams_of[5], 71), 0),
        "key_weight": noise(streams_of[1], (D, KVH * HD), D ** -0.5, 0.125),
        "value_weight": noise(streams_of[2], (D, KVH * HD), D ** -0.5, 0.125),
        "queries": noise(streams_of[3], (PAIRS, GROUP, HD), 1.0, 6.0, ((0, 32),)),
        "head_bias": draw_head_bias(jax.random.fold_in(streams_of[5], 71), 0),
    }


EPS_NORM = 0.0001

def reference(layer_input, key_weight, value_weight, queries, head_bias):
    tokens_flat = layer_input.reshape(SEQS * LEN, D)
    key_rows = jnp.dot(tokens_flat, key_weight, preferred_element_type=jnp.float32).astype(jnp.bfloat16).reshape(SEQS, LEN, KVH, HD)
    value_rows = jnp.dot(tokens_flat, value_weight, preferred_element_type=jnp.float32).astype(jnp.bfloat16).reshape(SEQS, LEN, KVH, HD)
    kv_rows = jnp.concatenate([key_rows, value_rows], axis=-1).transpose(0, 2, 1, 3).reshape(PAIRS, LEN, 2 * HD)
    head_shift = jnp.tile(head_bias, (SEQS, 1))
    score_scale = 1.0 / math.sqrt(HD)

    def read_pair(item):
        query, pair_rows, shift = item
        scores = jnp.dot(query, pair_rows[:, :HD].T, preferred_element_type=jnp.float32) * score_scale + shift[:, None]
        keep_log = jax.nn.log_sigmoid(-scores)
        suffix_log = lax.cumsum(keep_log, axis=1, reverse=True) - keep_log
        weights = jnp.exp(jax.nn.log_sigmoid(scores) + suffix_log).astype(jnp.bfloat16)
        return jnp.dot(weights, pair_rows[:, HD:], preferred_element_type=jnp.float32)
    summed = lax.map(read_pair, (queries, kv_rows, head_shift))
    squares = lax.optimization_barrier(jnp.mean(summed * summed, axis=-1, keepdims=True))
    first_read = (summed * lax.rsqrt(squares + EPS_NORM)).reshape(PAIRS, GROUP * HD).astype(jnp.bfloat16)
    return (kv_rows.reshape(PAIRS, BLOCKS, SPAN, 2 * HD), first_read)
```

```python
import functools
import math

import jax
import jax.numpy as jnp
from jax import lax
from jax.experimental import pallas as pl
from jax.experimental.pallas import tpu as pltpu
from jax.sharding import PartitionSpec as P


HD = 64
KVH = 6
GROUP = 5
LANES = 128
ROWS = 8

EPS_NORM = 0.0001
F32 = jnp.float32
BF16 = jnp.bfloat16


def lane_iota(shape):
    return lax.broadcasted_iota(jnp.int32, shape, len(shape) - 1)


def row_iota(shape):
    return lax.broadcasted_iota(jnp.int32, shape, len(shape) - 2)


def dot_01(x, ones):
    rows = x.shape[0]
    top = x.astype(BF16)
    rest = x - top.astype(F32)
    mid = rest.astype(BF16)
    low = (rest - mid.astype(F32)).astype(BF16)
    out = jnp.dot(jnp.concatenate([top, mid, low], axis=0), ones, preferred_element_type=F32)
    return out[:rows] + out[rows : 2 * rows] + out[2 * rows :]


def project_kernel(x_ref, w_ref, out_ref):
    acc = jnp.dot(x_ref[...], w_ref[...], preferred_element_type=F32)
    half = acc.shape[0] * KVH // out_ref.shape[0] // 2
    low_lanes = lane_iota((half, LANES)) < HD
    for s in range(acc.shape[0] // (2 * half)):
        for j in range(KVH // 2):
            first = acc[2 * s * half : (2 * s + 1) * half, j * LANES : (j + 1) * LANES]
            second = acc[(2 * s + 1) * half : (2 * s + 2) * half, j * LANES : (j + 1) * LANES]
            even = jnp.where(low_lanes, first, pltpu.roll(second, HD, 1))
            odd = jnp.where(low_lanes, pltpu.roll(first, HD, 1), second)
            out_ref[s * KVH + 2 * j] = even.astype(BF16)
            out_ref[s * KVH + 2 * j + 1] = odd.astype(BF16)


def project(tokens, weight, seq_count, positions, steps):
    rows, width = tokens.shape
    return pl.pallas_call(
        project_kernel,
        grid=(steps,),
        in_specs=[
            pl.BlockSpec((rows // steps, width), lambda i: (i, 0)),
            pl.BlockSpec(weight.shape, lambda i: (0, 0)),
        ],
        out_specs=pl.BlockSpec(
            (seq_count * KVH // steps, positions // 2, LANES), lambda i: (i, 0, 0)
        ),
        out_shape=jax.ShapeDtypeStruct((seq_count * KVH, positions // 2, LANES), BF16),
        cost_estimate=pl.CostEstimate(
            flops=2 * rows * width * weight.shape[1],
            bytes_accessed=2 * (rows * width + weight.size + rows * weight.shape[1]),
            transcendentals=0,
        ),
    )(tokens, weight)


def score_kernel(queries_ref, shift_ref, keys_ref, _, log_ref, totals_ref):
    blocks, pairs, half, _ = keys_ref.shape
    wide = blocks * half
    groups = wide // LANES
    keep_parts = []
    for i in range(pairs):
        keys = keys_ref[:, i].reshape(wide, LANES)
        scores = lax.dot_general(
            queries_ref[i], keys, (((1,), (1,)), ((), ())), preferred_element_type=F32
        ) * (1.0 / math.sqrt(HD)) + shift_ref[i]
        soft = jnp.log1p(jnp.exp(-jnp.abs(scores)))
        keep = jnp.minimum(-scores, 0.0) - soft
        log_ref[2 * ROWS * i : 2 * ROWS * (i + 1)] = jnp.minimum(scores, 0.0) - soft
        keep_parts.append(keep)
    stacked = jnp.concatenate(
        [k[:, n * LANES : (n + 1) * LANES] for k in keep_parts for n in range(groups)], axis=0
    )
    source = row_iota((LANES, 2 * LANES))
    target = lane_iota((LANES, 2 * LANES))
    place = target % LANES
    same = source // half == place // half
    later = (source > place) | (target >= LANES)
    sums = dot_01(stacked, jnp.where(same & later, 1.0, 0.0).astype(BF16))
    for i in range(pairs):
        for n in range(groups):
            at = (i * groups + n) * 2 * ROWS
            inside = sums[at : at + 2 * ROWS, :LANES]
            whole_high = sums[at + ROWS : at + 2 * ROWS, LANES:]
            cols = slice(n * LANES, (n + 1) * LANES)
            low_rows = slice(2 * ROWS * i, 2 * ROWS * i + ROWS)
            high_rows = slice(2 * ROWS * i + ROWS, 2 * ROWS * (i + 1))
            log_ref[low_rows, cols] += inside[:ROWS] + whole_high
            log_ref[high_rows, cols] += inside[ROWS:]
    both = jnp.concatenate([k[:ROWS] + k[ROWS:] for k in keep_parts], axis=0)
    member = row_iota((wide, LANES)) // half == lane_iota((wide, LANES))
    totals = dot_01(both, jnp.where(member, 1.0, 0.0).astype(BF16))
    totals_ref[...] = totals


def weight_kernel(blocks, me_ref, log_ref, own_ref, partner_ref, *rest):
    others, weights_ref = rest[:-1], rest[-1]
    rows = own_ref.shape[0]
    wide = log_ref.shape[1]
    half = wide // blocks
    core = me_ref[0] % 2
    chip = me_ref[0] // 2
    partner = partner_ref[...]
    chip_sums = own_ref[...] + partner
    later_inside = jnp.where(core == 0, partner, 0.0)
    block_sums = chip_sums
    for n, other_ref in enumerate(others):
        other = other_ref[...]
        later_inside = later_inside + jnp.where((chip ^ (n + 1)) > chip, other, 0.0)
        block_sums = block_sums + other
    after = row_iota((LANES, LANES)) > lane_iota((LANES, LANES))
    later_blocks = dot_01(block_sums, jnp.where(after, 1.0, 0.0).astype(BF16))
    member = row_iota((LANES, wide)) == lane_iota((LANES, wide)) // half
    later = dot_01(later_inside + later_blocks, jnp.where(member, 1.0, 0.0).astype(BF16))
    for i in range(rows // ROWS):
        for side in range(2):
            at = slice((2 * i + side) * ROWS, (2 * i + side + 1) * ROWS)
            weights_ref[at] = jnp.exp(log_ref[at] + later[i * ROWS : (i + 1) * ROWS]).astype(BF16)


def read_kernel(weights_ref, values_ref, out_ref):
    blocks, pairs, half, _ = values_ref.shape
    for i in range(pairs):
        values = values_ref[:, i].reshape(blocks * half, LANES)
        part = jnp.dot(
            weights_ref[2 * ROWS * i : 2 * ROWS * (i + 1)], values, preferred_element_type=F32
        )
        both = part[:ROWS] + pltpu.roll(part[ROWS:], HD, 1)
        out_ref[i * ROWS : (i + 1) * ROWS] = both


def norm_kernel(own_ref, first_ref, second_ref, third_ref, out_ref):
    summed = (own_ref[...] + first_ref[...]) + (second_ref[...] + third_ref[...])
    low_lanes = lane_iota(summed.shape) < HD
    summed = jnp.where(low_lanes, summed, 0.0)
    squares = jnp.sum(summed * summed, axis=-1, keepdims=True) * (1.0 / HD)
    normed = summed * lax.rsqrt(squares + EPS_NORM)
    swapped = pltpu.roll(normed, HD, 1)
    pairs = out_ref.shape[0]
    for j in range((GROUP + 1) // 2):
        rows = []
        for i in range(pairs):
            row = normed[i * ROWS + 2 * j : i * ROWS + 2 * j + 1]
            if 2 * j + 1 < GROUP:
                row = row + swapped[i * ROWS + 2 * j + 1 : i * ROWS + 2 * j + 2]
            rows.append(row)
        tile = jnp.concatenate(rows, axis=0).astype(BF16)
        width = min(LANES, GROUP * HD - j * LANES)
        out_ref[:, j * LANES : j * LANES + width] = tile[:, :width]


def store_kernel(keys_ref, values_ref, out_ref):
    _, pairs, half, _ = keys_ref.shape
    for i in range(pairs):
        keys = keys_ref[:, i]
        values = values_ref[:, i]
        out_ref[i, :, :half] = jnp.concatenate([keys[..., :HD], values[..., :HD]], axis=-1)
        out_ref[i, :, half:] = jnp.concatenate([keys[..., HD:], values[..., HD:]], axis=-1)


def call(kernel, out_shape, flops=0, in_specs=None):
    return pl.pallas_call(
        kernel,
        out_shape=out_shape,
        **({} if in_specs is None else {"in_specs": in_specs}),
        cost_estimate=pl.CostEstimate(flops=flops, bytes_accessed=0, transcendentals=0),
    )


def add_kernel(a_ref, b_ref, out_ref):
    out_ref[...] = a_ref[...] + b_ref[...]


def swap(x, distance):
    peers = lax.axis_size("tp")
    return lax.ppermute(x, "tp", [(i, i ^ distance) for i in range(peers)])


def cache_and_read(layer_input, key_weight, value_weight, queries, head_bias):
    seq_count, positions, model_width = layer_input.shape
    half = positions // 2
    pairs = queries.shape[0]
    blocks = lax.axis_size("sp")
    peers = lax.axis_size("tp")
    wide = blocks * half
    tokens = layer_input.reshape(seq_count * positions, model_width)

    keys_out = project(tokens, key_weight, seq_count, positions, 4)
    keys = lax.all_to_all(keys_out, "sp", split_axis=0, concat_axis=0, tiled=True)
    values_out = project(tokens, value_weight, seq_count, positions, 4)
    values = lax.all_to_all(values_out, "sp", split_axis=0, concat_axis=0, tiled=True)
    keys = keys.reshape(blocks, pairs, half, LANES)
    values = values.reshape(blocks, pairs, half, LANES)

    padded = jnp.pad(queries, ((0, 0), (0, ROWS - GROUP), (0, 0)))
    nothing = jnp.zeros_like(padded)
    two_sided = jnp.concatenate(
        [
            jnp.concatenate([padded, nothing], axis=2),
            jnp.concatenate([nothing, padded], axis=2),
        ],
        axis=1,
    )
    pair_ids = lax.axis_index("sp") * pairs + jnp.arange(pairs, dtype=jnp.int32)
    heads_range = jnp.arange(KVH, dtype=jnp.int32)
    picker = (pair_ids[:, None] % KVH == heads_range[None, :]).astype(F32)
    head_shift = jnp.dot(picker, head_bias, precision=lax.Precision.HIGHEST)
    head_shift = jnp.pad(head_shift, ((0, 0), (0, ROWS - GROUP)))
    head_shift = jnp.concatenate([head_shift, head_shift], axis=1)[:, :, None]

    whole = pl.BlockSpec(memory_space=pltpu.VMEM)
    log_weights, totals = call(
        score_kernel,
        (
            jax.ShapeDtypeStruct((pairs * 2 * ROWS, wide), F32),
            jax.ShapeDtypeStruct((pairs * ROWS, LANES), F32),
        ),
        flops=10**8,
        in_specs=[whole, whole, whole, pl.BlockSpec(memory_space=pl.ANY)],
    )(two_sided, head_shift, keys, values_out)
    small = jax.ShapeDtypeStruct((pairs * ROWS, LANES), F32)
    partner = swap(totals, 1)
    chip_totals = call(add_kernel, small)(totals, partner)
    others = [swap(chip_totals, 2 * n) for n in range(1, peers // 2)]
    me = lax.axis_index("tp").astype(jnp.int32).reshape(1)
    weights = call(
        functools.partial(weight_kernel, blocks),
        jax.ShapeDtypeStruct((pairs * 2 * ROWS, wide), BF16),
        flops=10**8,
        in_specs=[pl.BlockSpec(memory_space=pltpu.SMEM)] + [whole] * (3 + len(others)),
    )(me, log_weights, totals, partner, *others)
    part = call(read_kernel, small, flops=10**8)(weights, values)
    stored = call(
        store_kernel, jax.ShapeDtypeStruct((pairs, blocks, positions, LANES), BF16), flops=10**9
    )(keys, values)
    chip_part = call(add_kernel, small)(part, swap(part, 1))
    parts = [swap(chip_part, 2 * n) for n in range(1, peers // 2)]
    first_read = call(
        norm_kernel, jax.ShapeDtypeStruct((pairs, GROUP * HD), BF16), flops=10**6
    )(chip_part, *parts)
    return (stored, first_read)


def solution(mesh):
    in_specs = (P(None, ("sp", "tp"), None), P(), P(), P("sp", None, None), P())
    out_specs = (P("sp", None, "tp", None), P("sp", None))
    return jax.shard_map(
        cache_and_read, mesh=mesh, in_specs=in_specs, out_specs=out_specs, check_vma=False
    )
```

```python
import functools
import math

import jax
import jax.numpy as jnp
from jax import lax
from jax.experimental import pallas as pl
from jax.experimental.pallas import tpu as pltpu
from jax.sharding import PartitionSpec as P


HD = 64
KVH = 6
GROUP = 5
LANES = 128
ROWS = 8

EPS_NORM = 0.0001
VMEM_BYTES = 20 * 2**20
F32 = jnp.float32
BF16 = jnp.bfloat16


def lane_iota(shape):
    return lax.broadcasted_iota(jnp.int32, shape, len(shape) - 1)


def row_iota(shape):
    return lax.broadcasted_iota(jnp.int32, shape, len(shape) - 2)


def dot_01(x, ones):
    rows = x.shape[0]
    top = x.astype(BF16)
    rest = x - top.astype(F32)
    mid = rest.astype(BF16)
    low = (rest - mid.astype(F32)).astype(BF16)
    out = jnp.dot(jnp.concatenate([top, mid, low], axis=0), ones, preferred_element_type=F32)
    return out[:rows] + out[rows : 2 * rows] + out[2 * rows :]


def project_rows(acc, out_ref, first_seq, half):
    low_lanes = lane_iota((half, LANES)) < HD
    for s in range(acc.shape[0] // (2 * half)):
        for j in range(KVH // 2):
            cols = slice(j * LANES, (j + 1) * LANES)
            first = acc[2 * s * half : (2 * s + 1) * half, cols]
            second = acc[(2 * s + 1) * half : (2 * s + 2) * half, cols]
            even = jnp.where(low_lanes, first, pltpu.roll(second, HD, 1))
            odd = jnp.where(low_lanes, pltpu.roll(first, HD, 1), second)
            out_ref[(first_seq + s) * KVH + 2 * j] = even.astype(BF16)
            out_ref[(first_seq + s) * KVH + 2 * j + 1] = odd.astype(BF16)


def project_kernel(tokens_ref, weight_ref, out_ref, held, weight, row_sems, sems):
    rows, width = tokens_ref.shape
    half = out_ref.shape[1]
    parts = 4
    weight_copies = []
    for n in range(parts):
        at = slice(n * width // parts, (n + 1) * width // parts)
        copy = pltpu.make_async_copy(weight_ref.at[at], weight.at[at], sems.at[n])
        copy.start()
        weight_copies.append(copy)
    row_copies = []
    for n, at in enumerate((slice(0, rows // 4), slice(rows // 4, rows))):
        copy = pltpu.make_async_copy(tokens_ref.at[at], held.at[at], row_sems.at[n])
        copy.start()
        row_copies.append((at, copy))
    for copy in weight_copies:
        copy.wait()
    for at, copy in row_copies:
        copy.wait()
        acc = jnp.dot(held[at], weight[...], preferred_element_type=F32)
        project_rows(acc, out_ref, at.start // (2 * half), half)


def score_kernel(queries_ref, shift_ref, keys_ref, _, log_ref, totals_ref):
    blocks, pairs, half, _ = keys_ref.shape
    wide = blocks * half
    groups = wide // LANES
    keep_parts = []
    for i in range(pairs):
        keys = keys_ref[:, i].reshape(wide, LANES)
        scores = lax.dot_general(
            queries_ref[i], keys, (((1,), (1,)), ((), ())), preferred_element_type=F32
        ) * (1.0 / math.sqrt(HD)) + shift_ref[i]
        soft = jnp.log1p(jnp.exp(-jnp.abs(scores)))
        keep = jnp.minimum(-scores, 0.0) - soft
        log_ref[2 * ROWS * i : 2 * ROWS * (i + 1)] = jnp.minimum(scores, 0.0) - soft
        keep_parts.append(keep)
    stacked = jnp.concatenate(
        [k[:, n * LANES : (n + 1) * LANES] for k in keep_parts for n in range(groups)], axis=0
    )
    source = row_iota((LANES, 2 * LANES))
    target = lane_iota((LANES, 2 * LANES))
    place = target % LANES
    same = source // half == place // half
    later = (source > place) | (target >= LANES)
    sums = dot_01(stacked, jnp.where(same & later, 1.0, 0.0).astype(BF16))
    for i in range(pairs):
        for n in range(groups):
            at = (i * groups + n) * 2 * ROWS
            inside = sums[at : at + 2 * ROWS, :LANES]
            whole_high = sums[at + ROWS : at + 2 * ROWS, LANES:]
            cols = slice(n * LANES, (n + 1) * LANES)
            low_rows = slice(2 * ROWS * i, 2 * ROWS * i + ROWS)
            high_rows = slice(2 * ROWS * i + ROWS, 2 * ROWS * (i + 1))
            log_ref[low_rows, cols] += inside[:ROWS] + whole_high
            log_ref[high_rows, cols] += inside[ROWS:]
    both = jnp.concatenate([k[:ROWS] + k[ROWS:] for k in keep_parts], axis=0)
    member = row_iota((wide, LANES)) // half == lane_iota((wide, LANES))
    totals = dot_01(both, jnp.where(member, 1.0, 0.0).astype(BF16))
    totals_ref[...] = totals


def weight_kernel(blocks, me_ref, log_ref, own_ref, partner_ref, *rest):
    others, weights_ref = rest[:-1], rest[-1]
    rows = own_ref.shape[0]
    wide = log_ref.shape[1]
    half = wide // blocks
    core = me_ref[0] % 2
    chip = me_ref[0] // 2
    partner = partner_ref[...]
    chip_sums = own_ref[...] + partner
    later_inside = jnp.where(core == 0, partner, 0.0)
    block_sums = chip_sums
    for n, other_ref in enumerate(others):
        other = other_ref[...]
        later_inside = later_inside + jnp.where((chip ^ (n + 1)) > chip, other, 0.0)
        block_sums = block_sums + other
    after = row_iota((LANES, LANES)) > lane_iota((LANES, LANES))
    later_blocks = dot_01(block_sums, jnp.where(after, 1.0, 0.0).astype(BF16))
    member = row_iota((LANES, wide)) == lane_iota((LANES, wide)) // half
    later = dot_01(later_inside + later_blocks, jnp.where(member, 1.0, 0.0).astype(BF16))
    for i in range(rows // ROWS):
        for side in range(2):
            at = slice((2 * i + side) * ROWS, (2 * i + side + 1) * ROWS)
            weights_ref[at] = jnp.exp(log_ref[at] + later[i * ROWS : (i + 1) * ROWS]).astype(BF16)


def read_kernel(weights_ref, values_ref, out_ref):
    blocks, pairs, half, _ = values_ref.shape
    for i in range(pairs):
        values = values_ref[:, i].reshape(blocks * half, LANES)
        part = jnp.dot(
            weights_ref[2 * ROWS * i : 2 * ROWS * (i + 1)], values, preferred_element_type=F32
        )
        both = part[:ROWS] + pltpu.roll(part[ROWS:], HD, 1)
        out_ref[i * ROWS : (i + 1) * ROWS] = both


def norm_kernel(own_ref, first_ref, second_ref, third_ref, out_ref):
    summed = (own_ref[...] + first_ref[...]) + (second_ref[...] + third_ref[...])
    low_lanes = lane_iota(summed.shape) < HD
    summed = jnp.where(low_lanes, summed, 0.0)
    squares = jnp.sum(summed * summed, axis=-1, keepdims=True) * (1.0 / HD)
    normed = summed * lax.rsqrt(squares + EPS_NORM)
    swapped = pltpu.roll(normed, HD, 1)
    pairs = out_ref.shape[0]
    for j in range((GROUP + 1) // 2):
        rows = []
        for i in range(pairs):
            row = normed[i * ROWS + 2 * j : i * ROWS + 2 * j + 1]
            if 2 * j + 1 < GROUP:
                row = row + swapped[i * ROWS + 2 * j + 1 : i * ROWS + 2 * j + 2]
            rows.append(row)
        tile = jnp.concatenate(rows, axis=0).astype(BF16)
        width = min(LANES, GROUP * HD - j * LANES)
        out_ref[:, j * LANES : j * LANES + width] = tile[:, :width]


def store_kernel(keys_ref, values_ref, out_ref):
    _, pairs, half, _ = keys_ref.shape
    for i in range(pairs):
        keys = keys_ref[:, i]
        values = values_ref[:, i]
        out_ref[i, :, :half] = jnp.concatenate([keys[..., :HD], values[..., :HD]], axis=-1)
        out_ref[i, :, half:] = jnp.concatenate([keys[..., HD:], values[..., HD:]], axis=-1)


def in_vmem(x):
    return pltpu.with_memory_space_constraint(x, pltpu.VMEM)


def in_hbm(x):
    return pltpu.with_memory_space_constraint(x, pltpu.HBM)


def call(kernel, out_shape, flops=0, in_specs=None, scratch=()):
    return pl.pallas_call(
        kernel,
        out_shape=out_shape,
        **({} if in_specs is None else {"in_specs": in_specs}),
        scratch_shapes=scratch,
        compiler_params=pltpu.CompilerParams(vmem_limit_bytes=VMEM_BYTES),
        cost_estimate=pl.CostEstimate(flops=flops, bytes_accessed=0, transcendentals=0),
    )


def swap(x, distance):
    peers = lax.axis_size("tp")
    return lax.ppermute(x, "tp", [(i, i ^ distance) for i in range(peers)])


def cache_and_read(layer_input, key_weight, value_weight, queries, head_bias):
    seq_count, positions, model_width = layer_input.shape
    half = positions // 2
    pairs = queries.shape[0]
    blocks = lax.axis_size("sp")
    peers = lax.axis_size("tp")
    wide = blocks * half
    tokens = layer_input.reshape(seq_count * positions, model_width)

    def project(weight):
        return call(
            project_kernel,
            pltpu.VMEM((seq_count * KVH, half, LANES), BF16),
            flops=10**9,
            in_specs=[pl.BlockSpec(memory_space=pltpu.HBM)] * 2,
            scratch=[
                pltpu.VMEM(tokens.shape, BF16),
                pltpu.VMEM(weight.shape, BF16),
                pltpu.SemaphoreType.DMA((2,)),
                pltpu.SemaphoreType.DMA((4,)),
            ],
        )(in_hbm(tokens), in_hbm(weight))

    keys_out = project(key_weight)
    keys = lax.all_to_all(keys_out, "sp", split_axis=0, concat_axis=0, tiled=True)
    values_out = project(value_weight)
    values = lax.all_to_all(values_out, "sp", split_axis=0, concat_axis=0, tiled=True)
    keys = keys.reshape(blocks, pairs, half, LANES)
    values = values.reshape(blocks, pairs, half, LANES)

    padded = jnp.pad(queries, ((0, 0), (0, ROWS - GROUP), (0, 0)))
    nothing = jnp.zeros_like(padded)
    two_sided = jnp.concatenate(
        [
            jnp.concatenate([padded, nothing], axis=2),
            jnp.concatenate([nothing, padded], axis=2),
        ],
        axis=1,
    )
    pair_ids = lax.axis_index("sp") * pairs + jnp.arange(pairs, dtype=jnp.int32)
    heads_range = jnp.arange(KVH, dtype=jnp.int32)
    picker = (pair_ids[:, None] % KVH == heads_range[None, :]).astype(F32)
    head_shift = jnp.dot(picker, head_bias, precision=lax.Precision.HIGHEST)
    head_shift = jnp.pad(head_shift, ((0, 0), (0, ROWS - GROUP)))
    head_shift = jnp.concatenate([head_shift, head_shift], axis=1)[:, :, None]

    whole = pl.BlockSpec(memory_space=pltpu.VMEM)
    log_weights, totals = call(
        score_kernel,
        (
            pltpu.VMEM((pairs * 2 * ROWS, wide), F32),
            pltpu.VMEM((pairs * ROWS, LANES), F32),
        ),
        flops=10**8,
        in_specs=[whole, whole, whole, pl.BlockSpec(memory_space=pl.ANY)],
    )(in_vmem(two_sided), in_vmem(head_shift), in_vmem(keys), values_out)
    small = pltpu.VMEM((pairs * ROWS, LANES), F32)
    partner = swap(totals, 1)
    chip_totals = totals + partner
    others = [swap(chip_totals, 2 * n) for n in range(1, peers // 2)]
    me = lax.axis_index("tp").astype(jnp.int32).reshape(1)
    weights = call(
        functools.partial(weight_kernel, blocks),
        pltpu.VMEM((pairs * 2 * ROWS, wide), BF16),
        flops=10**8,
        in_specs=[pl.BlockSpec(memory_space=pltpu.SMEM)] + [whole] * (3 + len(others)),
    )(me, *(in_vmem(x) for x in (log_weights, totals, partner, *others)))
    part = call(read_kernel, small, flops=10**8)(in_vmem(weights), in_vmem(values))
    stored = call(
        store_kernel, jax.ShapeDtypeStruct((pairs, blocks, positions, LANES), BF16), flops=10**9
    )(in_vmem(keys), in_vmem(values))
    chip_part = part + swap(part, 1)
    parts = [swap(chip_part, 2 * n) for n in range(1, peers // 2)]
    first_read = call(
        norm_kernel, jax.ShapeDtypeStruct((pairs, GROUP * HD), BF16), flops=10**6
    )(*(in_vmem(x) for x in (chip_part, *parts)))
    return (stored, first_read)


def solution(mesh):
    in_specs = (P(None, ("sp", "tp"), None), P(), P(), P("sp", None, None), P())
    out_specs = (P("sp", None, "tp", None), P("sp", None))
    return jax.shard_map(
        cache_and_read, mesh=mesh, in_specs=in_specs, out_specs=out_specs, check_vma=False
    )
```

```python
import functools
import math

import jax
import jax.numpy as jnp
from jax import lax
from jax.experimental import pallas as pl
from jax.experimental.pallas import tpu as pltpu
from jax.sharding import PartitionSpec as P


HD = 64
KVH = 6
GROUP = 5
LANES = 128
ROWS = 8

EPS_NORM = 0.0001
VMEM_BYTES = 20 * 2**20
Z_ORDER = (4, 3, 5, 2, 6, 1, 7)
F32 = jnp.float32
BF16 = jnp.bfloat16


def lane_iota(shape):
    return lax.broadcasted_iota(jnp.int32, shape, len(shape) - 1)


def row_iota(shape):
    return lax.broadcasted_iota(jnp.int32, shape, len(shape) - 2)


def dot_01(x, ones):
    rows = x.shape[0]
    top = x.astype(BF16)
    rest = x - top.astype(F32)
    mid = rest.astype(BF16)
    low = (rest - mid.astype(F32)).astype(BF16)
    out = jnp.dot(jnp.concatenate([top, mid, low], axis=0), ones, preferred_element_type=F32)
    return out[:rows] + out[rows : 2 * rows] + out[2 * rows :]


DEPTH = 8
ACROSS = 4


def place():
    me = lax.axis_index("sp")
    return me // ACROSS, me % ACROSS


def project_rows(acc, out_ref, first_seq, half):
    low_lanes = lane_iota((half, LANES)) < HD
    pairs = out_ref.shape[-3]
    for s in range(acc.shape[0] // (2 * half)):
        for j in range(KVH // 2):
            cols = slice(j * LANES, (j + 1) * LANES)
            first = acc[2 * s * half : (2 * s + 1) * half, cols]
            second = acc[(2 * s + 1) * half : (2 * s + 2) * half, cols]
            even = jnp.where(low_lanes, first, pltpu.roll(second, HD, 1))
            odd = jnp.where(low_lanes, pltpu.roll(first, HD, 1), second)
            for n, rows in ((2 * j, even), (2 * j + 1, odd)):
                owner, i = divmod((first_seq + s) * KVH + n, pairs)
                out_ref[owner, i] = rows.astype(BF16)


def project_kernel(tokens_ref, key_weight_ref, value_weight_ref, keys_ref, *rest):
    value_refs = rest[:ACROSS]
    held, weights, keys, values, row_sems, weight_sems, out_sems = rest[ACROSS:]
    rows, width = tokens_ref.shape
    half = keys.shape[-2]
    _, x = place()
    parts = 4
    sources = (key_weight_ref, value_weight_ref)

    def load(side):
        copies = []
        for n in range(parts):
            at = slice(n * width // parts, (n + 1) * width // parts)
            copies.append(
                pltpu.make_async_copy(
                    sources[side].at[at], weights.at[side, at], weight_sems.at[side * parts + n]
                )
            )
            copies[-1].start()
        return copies

    key_copies = load(0)
    row_copies = []
    for n, at in enumerate((slice(0, rows // 4), slice(rows // 4, rows))):
        copy = pltpu.make_async_copy(tokens_ref.at[at], held.at[at], row_sems.at[n])
        copy.start()
        row_copies.append((at, copy))
    value_copies = load(1)
    for copy in key_copies:
        copy.wait()
    for at, copy in row_copies:
        copy.wait()
        acc = jnp.dot(held[at], weights[0], preferred_element_type=F32)
        project_rows(acc, keys, at.start // (2 * half), half)
    sends = [pltpu.make_async_copy(keys, keys_ref, out_sems.at[0])]
    sends[0].start()
    for copy in value_copies:
        copy.wait()
    acc = jnp.dot(held[...], weights[1], preferred_element_type=F32)
    project_rows(acc, values, 0, half)
    by_place = values.reshape(DEPTH, ACROSS, *values.shape[1:])
    for dx in range(ACROSS):
        send = pltpu.make_async_copy(
            by_place.at[:, (x + dx) % ACROSS], value_refs[dx], out_sems.at[1 + dx]
        )
        send.start()
        sends.append(send)
    for send in sends:
        send.wait()


def resort_kernel(*refs):
    ins, outs, sems = refs[:ACROSS], refs[ACROSS : ACROSS + DEPTH], refs[-1]
    z, _ = place()
    copies = []
    for dz in range(1, DEPTH):
        for dx in range(ACROSS):
            copy = pltpu.make_async_copy(
                ins[dx].at[(z + dz) % DEPTH], outs[dz].at[dx], sems.at[dz * ACROSS + dx]
            )
            copy.start()
            copies.append(copy)
    for dx in range(ACROSS):
        outs[0][dx] = ins[dx][z]
    for copy in copies:
        copy.wait()


def copy_kernel(in_ref, out_ref):
    out_ref[...] = in_ref[...]


def block_of(n):
    z, x = place()
    return (z + DEPTH - n // ACROSS) % DEPTH * ACROSS + (x + ACROSS - n % ACROSS) % ACROSS


def score_kernel(queries_ref, shift_ref, keys_ref, log_ref, totals_ref):
    blocks, pairs, half, _ = keys_ref.shape
    wide = blocks * half
    groups = wide // LANES
    keep_parts = []
    for i in range(pairs):
        keys = jnp.concatenate([keys_ref[block_of(n), i] for n in range(blocks)], axis=0)
        scores = lax.dot_general(
            queries_ref[i], keys, (((1,), (1,)), ((), ())), preferred_element_type=F32
        ) * (1.0 / math.sqrt(HD)) + shift_ref[i]
        soft = jnp.log1p(jnp.exp(-jnp.abs(scores)))
        keep = jnp.minimum(-scores, 0.0) - soft
        log_ref[2 * ROWS * i : 2 * ROWS * (i + 1)] = jnp.minimum(scores, 0.0) - soft
        keep_parts.append(keep)
    stacked = jnp.concatenate(
        [k[:, n * LANES : (n + 1) * LANES] for k in keep_parts for n in range(groups)], axis=0
    )
    source = row_iota((LANES, 2 * LANES))
    target = lane_iota((LANES, 2 * LANES))
    place = target % LANES
    same = source // half == place // half
    later = (source > place) | (target >= LANES)
    sums = dot_01(stacked, jnp.where(same & later, 1.0, 0.0).astype(BF16))
    for i in range(pairs):
        for n in range(groups):
            at = (i * groups + n) * 2 * ROWS
            inside = sums[at : at + 2 * ROWS, :LANES]
            whole_high = sums[at + ROWS : at + 2 * ROWS, LANES:]
            cols = slice(n * LANES, (n + 1) * LANES)
            low_rows = slice(2 * ROWS * i, 2 * ROWS * i + ROWS)
            high_rows = slice(2 * ROWS * i + ROWS, 2 * ROWS * (i + 1))
            log_ref[low_rows, cols] += inside[:ROWS] + whole_high
            log_ref[high_rows, cols] += inside[ROWS:]
    both = jnp.concatenate([k[:ROWS] + k[ROWS:] for k in keep_parts], axis=0)
    member = block_of(row_iota((wide, LANES)) // half) == lane_iota((wide, LANES))
    totals = dot_01(both, jnp.where(member, 1.0, 0.0).astype(BF16))
    totals_ref[...] = totals


def weight_kernel(blocks, log_ref, own_ref, partner_ref, near_ref, far_ref, weights_ref):
    rows = own_ref.shape[0]
    wide = log_ref.shape[1]
    half = wide // blocks
    me = lax.axis_index("tp")
    partner, near, far = partner_ref[...], near_ref[...], far_ref[...]
    block_sums = own_ref[...] + partner + near + far
    later_inside = (
        jnp.where(me % 2 == 0, partner, 0.0)
        + jnp.where(me // 2 % 2 == 0, near, 0.0)
        + jnp.where(me // 4 == 0, far, 0.0)
    )
    after = row_iota((LANES, LANES)) > lane_iota((LANES, LANES))
    later_blocks = dot_01(block_sums, jnp.where(after, 1.0, 0.0).astype(BF16))
    member = row_iota((LANES, wide)) == block_of(lane_iota((LANES, wide)) // half)
    later = dot_01(later_inside + later_blocks, jnp.where(member, 1.0, 0.0).astype(BF16))
    for i in range(rows // ROWS):
        for side in range(2):
            at = slice((2 * i + side) * ROWS, (2 * i + side + 1) * ROWS)
            weights_ref[at] = jnp.exp(log_ref[at] + later[i * ROWS : (i + 1) * ROWS]).astype(BF16)


def read_kernel(weights_ref, *refs):
    value_refs, out_ref = refs[:-1], refs[-1]
    across, pairs, half, _ = value_refs[0].shape
    for i in range(pairs):
        values = jnp.concatenate(
            [ref[:, i].reshape(across * half, LANES) for ref in value_refs], axis=0
        )
        part = jnp.dot(
            weights_ref[2 * ROWS * i : 2 * ROWS * (i + 1)], values, preferred_element_type=F32
        )
        both = part[:ROWS] + pltpu.roll(part[ROWS:], HD, 1)
        out_ref[i * ROWS : (i + 1) * ROWS] = both


def norm_kernel(near_ref, far_ref, out_ref):
    summed = near_ref[...] + far_ref[...]
    low_lanes = lane_iota(summed.shape) < HD
    summed = jnp.where(low_lanes, summed, 0.0)
    squares = jnp.sum(summed * summed, axis=-1, keepdims=True) * (1.0 / HD)
    normed = summed * lax.rsqrt(squares + EPS_NORM)
    swapped = pltpu.roll(normed, HD, 1)
    pairs = out_ref.shape[0]
    for j in range((GROUP + 1) // 2):
        rows = []
        for i in range(pairs):
            row = normed[i * ROWS + 2 * j : i * ROWS + 2 * j + 1]
            if 2 * j + 1 < GROUP:
                row = row + swapped[i * ROWS + 2 * j + 1 : i * ROWS + 2 * j + 2]
            rows.append(row)
        tile = jnp.concatenate(rows, axis=0).astype(BF16)
        width = min(LANES, GROUP * HD - j * LANES)
        out_ref[:, j * LANES : j * LANES + width] = tile[:, :width]


def store_kernel(keys_ref, *refs):
    value_refs, out_ref = refs[:-1], refs[-1]
    blocks, pairs, half, _ = keys_ref.shape
    for n in range(blocks):
        block = block_of(n)
        for i in range(pairs):
            keys = keys_ref[block, i]
            values = value_refs[n // ACROSS][n % ACROSS, i]
            out_ref[i, block, :half] = jnp.concatenate([keys[:, :HD], values[:, :HD]], axis=-1)
            out_ref[i, block, half:] = jnp.concatenate([keys[:, HD:], values[:, HD:]], axis=-1)


def in_vmem(x):
    return pltpu.with_memory_space_constraint(x, pltpu.VMEM)


def in_hbm(x):
    return pltpu.with_memory_space_constraint(x, pltpu.HBM)


def call(kernel, out_shape, flops=0, in_specs=None, out_specs=None, scratch=()):
    return pl.pallas_call(
        kernel,
        out_shape=out_shape,
        **({} if in_specs is None else {"in_specs": in_specs}),
        **({} if out_specs is None else {"out_specs": out_specs}),
        scratch_shapes=scratch,
        compiler_params=pltpu.CompilerParams(vmem_limit_bytes=VMEM_BYTES),
        cost_estimate=pl.CostEstimate(flops=flops, bytes_accessed=0, transcendentals=0),
    )


def swap(x, distance):
    peers = lax.axis_size("tp")
    return lax.ppermute(x, "tp", [(i, i ^ distance) for i in range(peers)])


def shift(x, dz, dx):
    pairs = [
        (z * ACROSS + c, (z + dz) % DEPTH * ACROSS + (c + dx) % ACROSS)
        for z in range(DEPTH)
        for c in range(ACROSS)
    ]
    return lax.ppermute(x, "sp", pairs)


def cache_and_read(layer_input, key_weight, value_weight, queries, head_bias):
    seq_count, positions, model_width = layer_input.shape
    half = positions // 2
    pairs = queries.shape[0]
    blocks = lax.axis_size("sp")
    wide = blocks * half
    tokens = layer_input.reshape(seq_count * positions, model_width)

    hbm = pl.BlockSpec(memory_space=pltpu.HBM)
    piece = (pairs, half, LANES)
    side = pltpu.VMEM((blocks, *piece), BF16)
    keys_out, *values = call(
        project_kernel,
        [pltpu.HBM((blocks, *piece), BF16)] + [pltpu.HBM((DEPTH, *piece), BF16)] * ACROSS,
        flops=10**9,
        in_specs=[hbm] * 3,
        out_specs=[hbm] * (1 + ACROSS),
        scratch=[
            pltpu.VMEM(tokens.shape, BF16),
            pltpu.VMEM((2, *key_weight.shape), BF16),
            side,
            side,
            pltpu.SemaphoreType.DMA((2,)),
            pltpu.SemaphoreType.DMA((8,)),
            pltpu.SemaphoreType.DMA((1 + ACROSS,)),
        ],
    )(in_hbm(tokens), in_hbm(key_weight), in_hbm(value_weight))
    for dx in range(1, ACROSS):
        values[dx] = shift(values[dx], 0, dx)
    keys = lax.all_to_all(keys_out, "sp", split_axis=0, concat_axis=0, tiled=True)
    values = call(
        resort_kernel,
        [pltpu.VMEM((ACROSS, *piece), BF16)]
        + [pltpu.HBM((ACROSS, *piece), BF16)] * (DEPTH - 1),
        flops=10**8,
        in_specs=[pl.BlockSpec(memory_space=pltpu.VMEM)] * ACROSS,
        out_specs=[pl.BlockSpec(memory_space=pltpu.VMEM)] + [hbm] * (DEPTH - 1),
        scratch=[pltpu.SemaphoreType.DMA((DEPTH * ACROSS,))],
    )(*values)
    values = list(values)
    for dz in Z_ORDER:
        values[dz] = shift(values[dz], dz, 0)

    padded = jnp.pad(queries, ((0, 0), (0, ROWS - GROUP), (0, 0)))
    nothing = jnp.zeros_like(padded)
    two_sided = jnp.concatenate(
        [
            jnp.concatenate([padded, nothing], axis=2),
            jnp.concatenate([nothing, padded], axis=2),
        ],
        axis=1,
    )
    pair_ids = lax.axis_index("sp") * pairs + jnp.arange(pairs, dtype=jnp.int32)
    heads_range = jnp.arange(KVH, dtype=jnp.int32)
    picker = (pair_ids[:, None] % KVH == heads_range[None, :]).astype(F32)
    head_shift = jnp.dot(picker, head_bias, precision=lax.Precision.HIGHEST)
    head_shift = jnp.pad(head_shift, ((0, 0), (0, ROWS - GROUP)))
    head_shift = jnp.concatenate([head_shift, head_shift], axis=1)[:, :, None]

    two_sided = call(copy_kernel, pltpu.VMEM(two_sided.shape, BF16), flops=1000)(in_vmem(two_sided))
    small = pltpu.VMEM((pairs * ROWS, LANES), F32)
    log_weights, totals = call(
        score_kernel, (pltpu.VMEM((pairs * 2 * ROWS, wide), F32), small), flops=10**8
    )(in_vmem(two_sided), in_vmem(head_shift), in_vmem(keys))
    partner = swap(totals, 1)
    chip_totals = totals + partner
    near = swap(chip_totals, 2)
    far = swap(chip_totals + near, 6)
    weights = call(
        functools.partial(weight_kernel, blocks),
        pltpu.VMEM((pairs * 2 * ROWS, wide), BF16),
        flops=10**8,
    )(*(in_vmem(x) for x in (log_weights, totals, partner, near, far)))
    held_values = [in_vmem(v) for v in values]
    part = call(read_kernel, small, flops=10**8)(in_vmem(weights), *held_values)
    stored = call(
        store_kernel, jax.ShapeDtypeStruct((pairs, blocks, positions, LANES), BF16), flops=10**8
    )(in_vmem(keys), *held_values)
    chip_part = part + swap(part, 1)
    near_part = chip_part + swap(chip_part, 2)
    first_read = call(
        norm_kernel, jax.ShapeDtypeStruct((pairs, GROUP * HD), BF16), flops=10**6
    )(in_vmem(near_part), in_vmem(swap(near_part, 6)))
    return (stored, first_read)


def solution(mesh):
    in_specs = (P(None, ("sp", "tp"), None), P(), P(), P("sp", None, None), P())
    out_specs = (P("sp", None, "tp", None), P("sp", None))
    return jax.shard_map(
        cache_and_read, mesh=mesh, in_specs=in_specs, out_specs=out_specs, check_vma=False
    )
```

```python
import functools
import math

import jax
import jax.numpy as jnp
from jax import lax
from jax.experimental import pallas as pl
from jax.experimental.pallas import tpu as pltpu
from jax.sharding import PartitionSpec as P


HD = 64
KVH = 6
GROUP = 5
LANES = 128
ROWS = 8

EPS_NORM = 0.0001
VMEM_BYTES = 20 * 2**20
Z_ORDER = (1, 7, 2, 6, 3, 5, 4)
F32 = jnp.float32
BF16 = jnp.bfloat16


def lane_iota(shape):
    return lax.broadcasted_iota(jnp.int32, shape, len(shape) - 1)


def row_iota(shape):
    return lax.broadcasted_iota(jnp.int32, shape, len(shape) - 2)


def dot_01(x, ones):
    rows = x.shape[0]
    top = x.astype(BF16)
    rest = x - top.astype(F32)
    mid = rest.astype(BF16)
    low = (rest - mid.astype(F32)).astype(BF16)
    out = jnp.dot(jnp.concatenate([top, mid, low], axis=0), ones, preferred_element_type=F32)
    return out[:rows] + out[rows : 2 * rows] + out[2 * rows :]


DEPTH = 8
ACROSS = 4


def place():
    me = lax.axis_index("sp")
    return me // ACROSS, me % ACROSS


def project_rows(acc, out_ref, first_seq, half):
    low_lanes = lane_iota((half, LANES)) < HD
    pairs = out_ref.shape[-3]
    for s in range(acc.shape[0] // (2 * half)):
        for j in range(KVH // 2):
            cols = slice(j * LANES, (j + 1) * LANES)
            first = acc[2 * s * half : (2 * s + 1) * half, cols]
            second = acc[(2 * s + 1) * half : (2 * s + 2) * half, cols]
            even = jnp.where(low_lanes, first, pltpu.roll(second, HD, 1))
            odd = jnp.where(low_lanes, pltpu.roll(first, HD, 1), second)
            for n, rows in ((2 * j, even), (2 * j + 1, odd)):
                owner, i = divmod((first_seq + s) * KVH + n, pairs)
                out_ref[owner, i] = rows.astype(BF16)


def project_kernel(tokens_ref, key_weight_ref, value_weight_ref, keys_ref, *rest):
    value_refs = rest[:ACROSS]
    held, weights, keys, values, row_sems, weight_sems, out_sems = rest[ACROSS:]
    rows, width = tokens_ref.shape
    half = keys.shape[-2]
    _, x = place()
    parts = 4
    sources = (key_weight_ref, value_weight_ref)

    def load(side):
        copies = []
        for n in range(parts):
            at = slice(n * width // parts, (n + 1) * width // parts)
            copies.append(
                pltpu.make_async_copy(
                    sources[side].at[at], weights.at[side, at], weight_sems.at[side * parts + n]
                )
            )
            copies[-1].start()
        return copies

    key_copies = load(0)
    row_copies = []
    for n, at in enumerate((slice(0, rows // 4), slice(rows // 4, rows))):
        copy = pltpu.make_async_copy(tokens_ref.at[at], held.at[at], row_sems.at[n])
        copy.start()
        row_copies.append((at, copy))
    value_copies = load(1)
    for copy in key_copies:
        copy.wait()
    for at, copy in row_copies:
        copy.wait()
        acc = jnp.dot(held[at], weights[0], preferred_element_type=F32)
        project_rows(acc, keys, at.start // (2 * half), half)
    sends = [pltpu.make_async_copy(keys, keys_ref, out_sems.at[0])]
    sends[0].start()
    for copy in value_copies:
        copy.wait()
    acc = jnp.dot(held[...], weights[1], preferred_element_type=F32)
    project_rows(acc, values, 0, half)
    for dx in range(ACROSS):
        for deep in range(DEPTH):
            value_refs[dx][deep] = values[deep * ACROSS + (x + dx) % ACROSS]
    for send in sends:
        send.wait()


def resort_kernel(*refs):
    ins, outs = refs[:ACROSS], refs[ACROSS:]
    z, _ = place()
    for dz in range(DEPTH):
        for dx in range(ACROSS):
            outs[dz][dx] = ins[dx][(z + dz) % DEPTH]


def copy_kernel(in_ref, out_ref):
    out_ref[...] = in_ref[...]


def block_of(n):
    z, x = place()
    return (z + DEPTH - n // ACROSS) % DEPTH * ACROSS + (x + ACROSS - n % ACROSS) % ACROSS


def score_kernel(queries_ref, shift_ref, keys_ref, log_ref, totals_ref):
    blocks, pairs, half, _ = keys_ref.shape
    wide = blocks * half
    groups = wide // LANES
    keep_parts = []
    for i in range(pairs):
        keys = jnp.concatenate([keys_ref[block_of(n), i] for n in range(blocks)], axis=0)
        scores = lax.dot_general(
            queries_ref[i], keys, (((1,), (1,)), ((), ())), preferred_element_type=F32
        ) * (1.0 / math.sqrt(HD)) + shift_ref[i]
        soft = jnp.log1p(jnp.exp(-jnp.abs(scores)))
        keep = jnp.minimum(-scores, 0.0) - soft
        log_ref[2 * ROWS * i : 2 * ROWS * (i + 1)] = jnp.minimum(scores, 0.0) - soft
        keep_parts.append(keep)
    stacked = jnp.concatenate(
        [k[:, n * LANES : (n + 1) * LANES] for k in keep_parts for n in range(groups)], axis=0
    )
    source = row_iota((LANES, 2 * LANES))
    target = lane_iota((LANES, 2 * LANES))
    place = target % LANES
    same = source // half == place // half
    later = (source > place) | (target >= LANES)
    sums = dot_01(stacked, jnp.where(same & later, 1.0, 0.0).astype(BF16))
    for i in range(pairs):
        for n in range(groups):
            at = (i * groups + n) * 2 * ROWS
            inside = sums[at : at + 2 * ROWS, :LANES]
            whole_high = sums[at + ROWS : at + 2 * ROWS, LANES:]
            cols = slice(n * LANES, (n + 1) * LANES)
            low_rows = slice(2 * ROWS * i, 2 * ROWS * i + ROWS)
            high_rows = slice(2 * ROWS * i + ROWS, 2 * ROWS * (i + 1))
            log_ref[low_rows, cols] += inside[:ROWS] + whole_high
            log_ref[high_rows, cols] += inside[ROWS:]
    both = jnp.concatenate([k[:ROWS] + k[ROWS:] for k in keep_parts], axis=0)
    member = block_of(row_iota((wide, LANES)) // half) == lane_iota((wide, LANES))
    totals = dot_01(both, jnp.where(member, 1.0, 0.0).astype(BF16))
    totals_ref[...] = totals


def weight_kernel(blocks, log_ref, own_ref, partner_ref, *rest):
    others, weights_ref = rest[:-1], rest[-1]
    rows = own_ref.shape[0]
    wide = log_ref.shape[1]
    half = wide // blocks
    me = lax.axis_index("tp")
    core, chip = me % 2, me // 2
    partner = partner_ref[...]
    block_sums = own_ref[...] + partner
    later_inside = jnp.where(core == 0, partner, 0.0)
    for n, other_ref in enumerate(others):
        other = other_ref[...]
        later_inside = later_inside + jnp.where((chip ^ (n + 1)) > chip, other, 0.0)
        block_sums = block_sums + other
    after = row_iota((LANES, LANES)) > lane_iota((LANES, LANES))
    later_blocks = dot_01(block_sums, jnp.where(after, 1.0, 0.0).astype(BF16))
    member = row_iota((LANES, wide)) == block_of(lane_iota((LANES, wide)) // half)
    later = dot_01(later_inside + later_blocks, jnp.where(member, 1.0, 0.0).astype(BF16))
    for i in range(rows // ROWS):
        for side in range(2):
            at = slice((2 * i + side) * ROWS, (2 * i + side + 1) * ROWS)
            weights_ref[at] = jnp.exp(log_ref[at] + later[i * ROWS : (i + 1) * ROWS]).astype(BF16)


def read_kernel(weights_ref, *refs):
    value_refs, out_ref = refs[:-1], refs[-1]
    across, pairs, half, _ = value_refs[0].shape
    for i in range(pairs):
        values = jnp.concatenate(
            [ref[:, i].reshape(across * half, LANES) for ref in value_refs], axis=0
        )
        part = jnp.dot(
            weights_ref[2 * ROWS * i : 2 * ROWS * (i + 1)], values, preferred_element_type=F32
        )
        both = part[:ROWS] + pltpu.roll(part[ROWS:], HD, 1)
        out_ref[i * ROWS : (i + 1) * ROWS] = both


def norm_kernel(own_ref, first_ref, second_ref, third_ref, out_ref):
    summed = (own_ref[...] + first_ref[...]) + (second_ref[...] + third_ref[...])
    low_lanes = lane_iota(summed.shape) < HD
    summed = jnp.where(low_lanes, summed, 0.0)
    squares = jnp.sum(summed * summed, axis=-1, keepdims=True) * (1.0 / HD)
    normed = summed * lax.rsqrt(squares + EPS_NORM)
    swapped = pltpu.roll(normed, HD, 1)
    pairs = out_ref.shape[0]
    for j in range((GROUP + 1) // 2):
        rows = []
        for i in range(pairs):
            row = normed[i * ROWS + 2 * j : i * ROWS + 2 * j + 1]
            if 2 * j + 1 < GROUP:
                row = row + swapped[i * ROWS + 2 * j + 1 : i * ROWS + 2 * j + 2]
            rows.append(row)
        tile = jnp.concatenate(rows, axis=0).astype(BF16)
        width = min(LANES, GROUP * HD - j * LANES)
        out_ref[:, j * LANES : j * LANES + width] = tile[:, :width]


def store_kernel(keys_ref, *refs):
    value_refs, out_ref = refs[:-1], refs[-1]
    blocks, pairs, half, _ = keys_ref.shape
    for n in range(blocks):
        block = block_of(n)
        for i in range(pairs):
            keys = keys_ref[block, i]
            values = value_refs[n // ACROSS][n % ACROSS, i]
            out_ref[i, block, :half] = jnp.concatenate([keys[:, :HD], values[:, :HD]], axis=-1)
            out_ref[i, block, half:] = jnp.concatenate([keys[:, HD:], values[:, HD:]], axis=-1)


def in_vmem(x):
    return pltpu.with_memory_space_constraint(x, pltpu.VMEM)


def in_hbm(x):
    return pltpu.with_memory_space_constraint(x, pltpu.HBM)


def call(kernel, out_shape, flops=0, in_specs=None, out_specs=None, scratch=()):
    return pl.pallas_call(
        kernel,
        out_shape=out_shape,
        **({} if in_specs is None else {"in_specs": in_specs}),
        **({} if out_specs is None else {"out_specs": out_specs}),
        scratch_shapes=scratch,
        compiler_params=pltpu.CompilerParams(vmem_limit_bytes=VMEM_BYTES),
        cost_estimate=pl.CostEstimate(flops=flops, bytes_accessed=0, transcendentals=0),
    )


def swap(x, distance):
    peers = lax.axis_size("tp")
    return lax.ppermute(x, "tp", [(i, i ^ distance) for i in range(peers)])


def shift(x, dz, dx):
    pairs = [
        (z * ACROSS + c, (z + dz) % DEPTH * ACROSS + (c + dx) % ACROSS)
        for z in range(DEPTH)
        for c in range(ACROSS)
    ]
    return lax.ppermute(x, "sp", pairs)


def cache_and_read(layer_input, key_weight, value_weight, queries, head_bias):
    seq_count, positions, model_width = layer_input.shape
    half = positions // 2
    pairs = queries.shape[0]
    blocks = lax.axis_size("sp")
    wide = blocks * half
    tokens = layer_input.reshape(seq_count * positions, model_width)

    hbm = pl.BlockSpec(memory_space=pltpu.HBM)
    piece = (pairs, half, LANES)
    side = pltpu.VMEM((blocks, *piece), BF16)
    keys_out, *values = call(
        project_kernel,
        [pltpu.HBM((blocks, *piece), BF16)] + [pltpu.VMEM((DEPTH, *piece), BF16)] * ACROSS,
        flops=10**9,
        in_specs=[hbm] * 3,
        out_specs=[hbm] + [pl.BlockSpec(memory_space=pltpu.VMEM)] * ACROSS,
        scratch=[
            pltpu.VMEM(tokens.shape, BF16),
            pltpu.VMEM((2, *key_weight.shape), BF16),
            side,
            side,
            pltpu.SemaphoreType.DMA((2,)),
            pltpu.SemaphoreType.DMA((8,)),
            pltpu.SemaphoreType.DMA((1,)),
        ],
    )(in_hbm(tokens), in_hbm(key_weight), in_hbm(value_weight))
    for dx in range(1, ACROSS):
        values[dx] = shift(values[dx], 0, dx)
    keys = lax.all_to_all(keys_out, "sp", split_axis=0, concat_axis=0, tiled=True)
    values = call(
        resort_kernel, [pltpu.VMEM((ACROSS, *piece), BF16)] * DEPTH, flops=10**8
    )(*(in_vmem(v) for v in values))
    values = list(values)
    for dz in Z_ORDER:
        values[dz] = shift(values[dz], dz, 0)

    padded = jnp.pad(queries, ((0, 0), (0, ROWS - GROUP), (0, 0)))
    nothing = jnp.zeros_like(padded)
    two_sided = jnp.concatenate(
        [
            jnp.concatenate([padded, nothing], axis=2),
            jnp.concatenate([nothing, padded], axis=2),
        ],
        axis=1,
    )
    pair_ids = lax.axis_index("sp") * pairs + jnp.arange(pairs, dtype=jnp.int32)
    heads_range = jnp.arange(KVH, dtype=jnp.int32)
    picker = (pair_ids[:, None] % KVH == heads_range[None, :]).astype(F32)
    head_shift = jnp.dot(picker, head_bias, precision=lax.Precision.HIGHEST)
    head_shift = jnp.pad(head_shift, ((0, 0), (0, ROWS - GROUP)))
    head_shift = jnp.concatenate([head_shift, head_shift], axis=1)[:, :, None]

    two_sided = call(copy_kernel, pltpu.VMEM(two_sided.shape, BF16), flops=1000)(in_vmem(two_sided))
    small = pltpu.VMEM((pairs * ROWS, LANES), F32)
    log_weights, totals = call(
        score_kernel, (pltpu.VMEM((pairs * 2 * ROWS, wide), F32), small), flops=10**8
    )(in_vmem(two_sided), in_vmem(head_shift), in_vmem(keys))
    partner = swap(totals, 1)
    chip_totals = totals + partner
    others = [swap(chip_totals, 2 * n) for n in range(1, lax.axis_size("tp") // 2)]
    weights = call(
        functools.partial(weight_kernel, blocks),
        pltpu.VMEM((pairs * 2 * ROWS, wide), BF16),
        flops=10**8,
    )(*(in_vmem(x) for x in (log_weights, totals, partner, *others)))
    held_values = [in_vmem(v) for v in values]
    part = call(read_kernel, small, flops=10**8)(in_vmem(weights), *held_values)
    stored = call(
        store_kernel, jax.ShapeDtypeStruct((pairs, blocks, positions, LANES), BF16), flops=10**8
    )(in_vmem(keys), *held_values)
    chip_part = part + swap(part, 1)
    parts = [swap(chip_part, 2 * n) for n in range(1, lax.axis_size("tp") // 2)]
    first_read = call(
        norm_kernel, jax.ShapeDtypeStruct((pairs, GROUP * HD), BF16), flops=10**6
    )(*(in_vmem(x) for x in (chip_part, *parts)))
    return (stored, first_read)


def solution(mesh):
    in_specs = (P(None, ("sp", "tp"), None), P(), P(), P("sp", None, None), P())
    out_specs = (P("sp", None, "tp", None), P("sp", None))
    return jax.shard_map(
        cache_and_read, mesh=mesh, in_specs=in_specs, out_specs=out_specs, check_vma=False
    )
```

```python
import functools
import math

import jax
import jax.numpy as jnp
from jax import lax
from jax.experimental import pallas as pl
from jax.experimental.pallas import tpu as pltpu
from jax.sharding import PartitionSpec as P


HD = 64
KVH = 6
GROUP = 5
LANES = 128
ROWS = 8

EPS_NORM = 0.0001
VMEM_BYTES = 20 * 2**20
NEAR = (2, 6, 3, 5, 7, 1)
FAR = (4,)
F32 = jnp.float32
BF16 = jnp.bfloat16


def lane_iota(shape):
    return lax.broadcasted_iota(jnp.int32, shape, len(shape) - 1)


def row_iota(shape):
    return lax.broadcasted_iota(jnp.int32, shape, len(shape) - 2)


def dot_01(x, ones):
    rows = x.shape[0]
    top = x.astype(BF16)
    rest = x - top.astype(F32)
    mid = rest.astype(BF16)
    low = (rest - mid.astype(F32)).astype(BF16)
    out = jnp.dot(jnp.concatenate([top, mid, low], axis=0), ones, preferred_element_type=F32)
    return out[:rows] + out[rows : 2 * rows] + out[2 * rows :]


DEPTH = 8
ACROSS = 4
ACROSS_BITS = 2


def place():
    me = lax.axis_index("sp")
    return me >> ACROSS_BITS, me & (ACROSS - 1)


def owner_at(dz, dx):
    z, x = place()
    return (((z + dz) & (DEPTH - 1)) << ACROSS_BITS) + ((x + dx) & (ACROSS - 1))


def project_rows(acc, out_ref, first_seq, half):
    low_lanes = lane_iota((half, LANES)) < HD
    pairs = out_ref.shape[-3]
    for s in range(acc.shape[0] // (2 * half)):
        for j in range(KVH // 2):
            cols = slice(j * LANES, (j + 1) * LANES)
            first = acc[2 * s * half : (2 * s + 1) * half, cols]
            second = acc[(2 * s + 1) * half : (2 * s + 2) * half, cols]
            even = jnp.where(low_lanes, first, pltpu.roll(second, HD, 1))
            odd = jnp.where(low_lanes, pltpu.roll(first, HD, 1), second)
            for n, rows in ((2 * j, even), (2 * j + 1, odd)):
                owner, i = divmod((first_seq + s) * KVH + n, pairs)
                out_ref[owner, i] = rows.astype(BF16)


def project_kernel(tokens_ref, key_weight_ref, value_weight_ref, keys_ref, *rest):
    near_refs, far_refs = rest[:ACROSS], rest[ACROSS : ACROSS + len(FAR)]
    held, weights, keys, values, row_sems, weight_sems, out_sems = rest[ACROSS + len(FAR) :]
    rows, width = tokens_ref.shape
    half = keys.shape[-2]
    parts = 4
    cols = key_weight_ref.shape[1]
    copies = []
    for side, source in enumerate((key_weight_ref, value_weight_ref)):
        for n in range(parts):
            at = slice(n * width // parts, (n + 1) * width // parts)
            copies.append(
                pltpu.make_async_copy(
                    source.at[at],
                    weights.at[at, side * cols : (side + 1) * cols],
                    weight_sems.at[side * parts + n],
                )
            )
            copies[-1].start()
    row_copies = []
    for n, at in enumerate((slice(0, rows // 4), slice(rows // 4, rows))):
        copy = pltpu.make_async_copy(tokens_ref.at[at], held.at[at], row_sems.at[n])
        copy.start()
        row_copies.append((at, copy))
    for copy in copies:
        copy.wait()
    for at, copy in row_copies:
        copy.wait()
        acc = jnp.dot(held[at], weights[...], preferred_element_type=F32)
        project_rows(acc[:, :cols], keys, at.start // (2 * half), half)
        project_rows(acc[:, cols:], values, at.start // (2 * half), half)
    sends = [pltpu.make_async_copy(keys, keys_ref, out_sems.at[0])]
    sends[0].start()
    for dx in range(ACROSS):
        for n, dz in enumerate((0, *NEAR)):
            near_refs[dx][n] = values[owner_at(dz, dx)]
        for far_ref, dz in zip(far_refs, FAR):
            far_ref[dx] = values[owner_at(dz, dx)]
    for send in sends:
        send.wait()


def resort_kernel(count, *refs):
    ins, outs = refs[:count], refs[count:]
    for m, in_ref in enumerate(ins):
        for n, out_ref in enumerate(outs):
            out_ref[m] = in_ref[n]


def copy_kernel(in_ref, out_ref):
    out_ref[...] = in_ref[...]


def block_of(n):
    z, x = place()
    deep = (z - (n >> ACROSS_BITS)) & (DEPTH - 1)
    return (deep << ACROSS_BITS) + ((x - n) & (ACROSS - 1))


def score_kernel(queries_ref, shift_ref, keys_ref, log_ref, totals_ref):
    blocks, pairs, half, _ = keys_ref.shape
    wide = blocks * half
    groups = wide // LANES
    keep_parts = []
    for i in range(pairs):
        keys = jnp.concatenate([keys_ref[block_of(n), i] for n in range(blocks)], axis=0)
        scores = lax.dot_general(
            queries_ref[i], keys, (((1,), (1,)), ((), ())), preferred_element_type=F32
        ) * (1.0 / math.sqrt(HD)) + shift_ref[i]
        soft = jnp.log1p(jnp.exp(-jnp.abs(scores)))
        keep = jnp.minimum(-scores, 0.0) - soft
        log_ref[2 * ROWS * i : 2 * ROWS * (i + 1)] = jnp.minimum(scores, 0.0) - soft
        keep_parts.append(keep)
    stacked = jnp.concatenate(
        [k[:, n * LANES : (n + 1) * LANES] for k in keep_parts for n in range(groups)], axis=0
    )
    source = row_iota((LANES, 2 * LANES))
    target = lane_iota((LANES, 2 * LANES))
    place = target % LANES
    same = source // half == place // half
    later = (source > place) | (target >= LANES)
    sums = dot_01(stacked, jnp.where(same & later, 1.0, 0.0).astype(BF16))
    for i in range(pairs):
        for n in range(groups):
            at = (i * groups + n) * 2 * ROWS
            inside = sums[at : at + 2 * ROWS, :LANES]
            whole_high = sums[at + ROWS : at + 2 * ROWS, LANES:]
            cols = slice(n * LANES, (n + 1) * LANES)
            low_rows = slice(2 * ROWS * i, 2 * ROWS * i + ROWS)
            high_rows = slice(2 * ROWS * i + ROWS, 2 * ROWS * (i + 1))
            log_ref[low_rows, cols] += inside[:ROWS] + whole_high
            log_ref[high_rows, cols] += inside[ROWS:]
    both = jnp.concatenate([k[:ROWS] + k[ROWS:] for k in keep_parts], axis=0)
    member = block_of(row_iota((wide, LANES)) // half) == lane_iota((wide, LANES))
    totals = dot_01(both, jnp.where(member, 1.0, 0.0).astype(BF16))
    totals_ref[...] = totals


def weight_kernel(blocks, log_ref, own_ref, partner_ref, *rest):
    others, weights_ref = rest[:-1], rest[-1]
    rows = own_ref.shape[0]
    wide = log_ref.shape[1]
    half = wide // blocks
    me = lax.axis_index("tp")
    core, chip = me % 2, me // 2
    partner = partner_ref[...]
    block_sums = own_ref[...] + partner
    later_inside = jnp.where(core == 0, partner, 0.0)
    for n, other_ref in enumerate(others):
        other = other_ref[...]
        later_inside = later_inside + jnp.where((chip ^ (n + 1)) > chip, other, 0.0)
        block_sums = block_sums + other
    after = row_iota((LANES, LANES)) > lane_iota((LANES, LANES))
    later_blocks = dot_01(block_sums, jnp.where(after, 1.0, 0.0).astype(BF16))
    member = row_iota((LANES, wide)) == block_of(lane_iota((LANES, wide)) // half)
    later = dot_01(later_inside + later_blocks, jnp.where(member, 1.0, 0.0).astype(BF16))
    for i in range(rows // ROWS):
        for side in range(2):
            at = slice((2 * i + side) * ROWS, (2 * i + side + 1) * ROWS)
            weights_ref[at] = jnp.exp(log_ref[at] + later[i * ROWS : (i + 1) * ROWS]).astype(BF16)


def values_of(refs):
    near, far = refs[: 1 + len(NEAR)], refs[1 + len(NEAR) :]
    order = (0, *NEAR)
    return [
        (near[order.index(dz)], dx) if dz in order else (far[dx], FAR.index(dz))
        for dz in range(DEPTH)
        for dx in range(ACROSS)
    ]


def read_kernel(weights_ref, *refs):
    pieces, out_ref = values_of(refs[:-1]), refs[-1]
    pairs = refs[0].shape[1]
    for i in range(pairs):
        values = jnp.concatenate([ref[n, i] for ref, n in pieces], axis=0)
        part = jnp.dot(
            weights_ref[2 * ROWS * i : 2 * ROWS * (i + 1)], values, preferred_element_type=F32
        )
        both = part[:ROWS] + pltpu.roll(part[ROWS:], HD, 1)
        out_ref[i * ROWS : (i + 1) * ROWS] = both


def norm_kernel(own_ref, first_ref, second_ref, third_ref, out_ref):
    summed = (own_ref[...] + first_ref[...]) + (second_ref[...] + third_ref[...])
    low_lanes = lane_iota(summed.shape) < HD
    summed = jnp.where(low_lanes, summed, 0.0)
    squares = jnp.sum(summed * summed, axis=-1, keepdims=True) * (1.0 / HD)
    normed = summed * lax.rsqrt(squares + EPS_NORM)
    swapped = pltpu.roll(normed, HD, 1)
    pairs = out_ref.shape[0]
    for j in range((GROUP + 1) // 2):
        rows = []
        for i in range(pairs):
            row = normed[i * ROWS + 2 * j : i * ROWS + 2 * j + 1]
            if 2 * j + 1 < GROUP:
                row = row + swapped[i * ROWS + 2 * j + 1 : i * ROWS + 2 * j + 2]
            rows.append(row)
        tile = jnp.concatenate(rows, axis=0).astype(BF16)
        width = min(LANES, GROUP * HD - j * LANES)
        out_ref[:, j * LANES : j * LANES + width] = tile[:, :width]


def store_kernel(keys_ref, *refs):
    pieces, out_ref = values_of(refs[:-1]), refs[-1]
    _, pairs, half, _ = keys_ref.shape
    for n, (ref, at) in enumerate(pieces):
        block = block_of(n)
        for i in range(pairs):
            keys = keys_ref[block, i]
            values = ref[at, i]
            out_ref[i, block, :half] = jnp.concatenate([keys[:, :HD], values[:, :HD]], axis=-1)
            out_ref[i, block, half:] = jnp.concatenate([keys[:, HD:], values[:, HD:]], axis=-1)


def in_vmem(x):
    return pltpu.with_memory_space_constraint(x, pltpu.VMEM)


def in_hbm(x):
    return pltpu.with_memory_space_constraint(x, pltpu.HBM)


def call(kernel, out_shape, flops=0, in_specs=None, out_specs=None, scratch=()):
    return pl.pallas_call(
        kernel,
        out_shape=out_shape,
        **({} if in_specs is None else {"in_specs": in_specs}),
        **({} if out_specs is None else {"out_specs": out_specs}),
        scratch_shapes=scratch,
        compiler_params=pltpu.CompilerParams(vmem_limit_bytes=VMEM_BYTES),
        cost_estimate=pl.CostEstimate(flops=flops, bytes_accessed=0, transcendentals=0),
    )


def swap(x, distance):
    peers = lax.axis_size("tp")
    return lax.ppermute(x, "tp", [(i, i ^ distance) for i in range(peers)])


def shift(x, dz, dx):
    pairs = [
        (z * ACROSS + c, (z + dz) % DEPTH * ACROSS + (c + dx) % ACROSS)
        for z in range(DEPTH)
        for c in range(ACROSS)
    ]
    return lax.ppermute(x, "sp", pairs)


def swap_chips(x):
    others = {n: swap(x, 2 * n) for n in (2, 1, 3)}
    return [others[n] for n in (1, 2, 3)]


def cache_and_read(layer_input, key_weight, value_weight, queries, head_bias):
    seq_count, positions, model_width = layer_input.shape
    half = positions // 2
    pairs = queries.shape[0]
    blocks = lax.axis_size("sp")
    wide = blocks * half
    tokens = layer_input.reshape(seq_count * positions, model_width)

    hbm = pl.BlockSpec(memory_space=pltpu.HBM)
    piece = (pairs, half, LANES)
    side = pltpu.VMEM((blocks, *piece), BF16)
    deep = 1 + len(NEAR)
    keys_out, *values = call(
        project_kernel,
        [pltpu.HBM((blocks, *piece), BF16)]
        + [pltpu.VMEM((deep, *piece), BF16)] * ACROSS
        + [pltpu.VMEM((ACROSS, *piece), BF16)] * len(FAR),
        flops=10**9,
        in_specs=[hbm] * 3,
        out_specs=[hbm] + [pl.BlockSpec(memory_space=pltpu.VMEM)] * (ACROSS + len(FAR)),
        scratch=[
            pltpu.VMEM(tokens.shape, BF16),
            pltpu.VMEM((model_width, 2 * key_weight.shape[1]), BF16),
            side,
            side,
            pltpu.SemaphoreType.DMA((2,)),
            pltpu.SemaphoreType.DMA((8,)),
            pltpu.SemaphoreType.DMA((1,)),
        ],
    )(in_hbm(tokens), in_hbm(key_weight), in_hbm(value_weight))
    near, far = values[:ACROSS], values[ACROSS:]
    for n, dz in enumerate(FAR):
        far[n] = shift(far[n], dz, 0)
    for dx in range(1, ACROSS):
        near[dx] = shift(near[dx], 0, dx)
    keys = lax.all_to_all(keys_out, "sp", split_axis=0, concat_axis=0, tiled=True)

    def resort(ins, count):
        return list(
            call(
                functools.partial(resort_kernel, len(ins)),
                [pltpu.VMEM((len(ins), *piece), BF16)] * count,
                flops=10**8,
            )(*(in_vmem(v) for v in ins))
        )

    near = resort(near, deep)
    for n, dz in enumerate(NEAR):
        near[1 + n] = shift(near[1 + n], dz, 0)
    far = resort(far, ACROSS)
    for dx in range(1, ACROSS):
        far[dx] = shift(far[dx], 0, dx)
    values = near + far

    padded = jnp.pad(queries, ((0, 0), (0, ROWS - GROUP), (0, 0)))
    nothing = jnp.zeros_like(padded)
    two_sided = jnp.concatenate(
        [
            jnp.concatenate([padded, nothing], axis=2),
            jnp.concatenate([nothing, padded], axis=2),
        ],
        axis=1,
    )
    pair_ids = lax.axis_index("sp") * pairs + jnp.arange(pairs, dtype=jnp.int32)
    heads_range = jnp.arange(KVH, dtype=jnp.int32)
    picker = (pair_ids[:, None] % KVH == heads_range[None, :]).astype(F32)
    head_shift = jnp.dot(picker, head_bias, precision=lax.Precision.HIGHEST)
    head_shift = jnp.pad(head_shift, ((0, 0), (0, ROWS - GROUP)))
    head_shift = jnp.concatenate([head_shift, head_shift], axis=1)[:, :, None]

    two_sided = call(copy_kernel, pltpu.VMEM(two_sided.shape, BF16), flops=1000)(in_vmem(two_sided))
    small = pltpu.VMEM((pairs * ROWS, LANES), F32)
    log_weights, totals = call(
        score_kernel, (pltpu.VMEM((pairs * 2 * ROWS, wide), F32), small), flops=10**8
    )(in_vmem(two_sided), in_vmem(head_shift), in_vmem(keys))
    partner = swap(totals, 1)
    chip_totals = totals + partner
    others = swap_chips(chip_totals)
    weights = call(
        functools.partial(weight_kernel, blocks),
        pltpu.VMEM((pairs * 2 * ROWS, wide), BF16),
        flops=10**8,
    )(*(in_vmem(x) for x in (log_weights, totals, partner, *others)))
    held_values = [in_vmem(v) for v in values]
    part = call(read_kernel, small, flops=10**8)(in_vmem(weights), *held_values)
    stored = call(
        store_kernel, jax.ShapeDtypeStruct((pairs, blocks, positions, LANES), BF16), flops=10**8
    )(in_vmem(keys), *held_values)
    chip_part = part + swap(part, 1)
    parts = swap_chips(chip_part)
    first_read = call(
        norm_kernel, jax.ShapeDtypeStruct((pairs, GROUP * HD), BF16), flops=10**6
    )(*(in_vmem(x) for x in (chip_part, *parts)))
    return (stored, first_read)


def solution(mesh):
    in_specs = (P(None, ("sp", "tp"), None), P(), P(), P("sp", None, None), P())
    out_specs = (P("sp", None, "tp", None), P("sp", None))
    return jax.shard_map(
        cache_and_read, mesh=mesh, in_specs=in_specs, out_specs=out_specs, check_vma=False
    )
```
